32 devices in a mesh: ra: 8 (over z, x), cb: 4 (over y, core).
Axes of the slice: x: 2, y: 2, z: 4, core: 2. Of those that a mesh axis runs over, the one named last changes fastest.
Arguments:
- stream: bfloat16 [128, 2048], P(None, 'ra'), may hold values from -6 to 6
- gain_first: float32 [2048], P('ra'), may hold values from 0.5 to 1.5
- lift_first: bfloat16 [2048, 8192], P('ra', 'cb'), may hold values from -0.125 to 0.125
- drop_first: bfloat16 [8192, 2048], P('cb', 'ra'), may hold values from -0.0625 to 0.0625
- gain_second: float32 [2048], P('ra'), may hold values from 0.5 to 1.5
- lift_second: bfloat16 [2048, 8192], P('ra', 'cb'), may hold values from -0.125 to 0.125
- drop_second: bfloat16 [8192, 2048], P('cb', 'ra'), may hold values from -0.0625 to 0.0625
Outputs:
- stream_out: bfloat16 [128, 2048], P(None, 'ra')
The draws below stay inside these ranges and needn't reach their ends.
All inputs are finite; a program needn't handle non-finite values.
Results may differ from the reference program's by a relative error of at most 0.0075.
Values may be sent and summed in bfloat16 or wider, within the bound.
A program may use at most 64 MiB of HBM per device.

```python
import jax
import jax.numpy as jnp
from jax import lax

D = 2048
HIDDEN_SIZE = 8192
TOKENS = 128


def level_of(own_key, extent, split, low, largest):
    loudness, own = 1.0, jax.random.fold_in(own_key, 6)
    for dim, blocks in split:
        draws = jnp.exp(jax.random.uniform(jax.random.fold_in(own, dim), (blocks,), jnp.float32, low / len(split), largest / len(split)))
        loudness = loudness * jnp.repeat(draws, extent[dim] // blocks).reshape([-1 if axis == dim else 1 for axis in range(len(extent))])
    return loudness


def noise(stream_key, shape, width, bound, cuts=(), kind=jnp.bfloat16):
    array = jax.random.normal(stream_key, shape, jnp.float32) * width
    if len(cuts) > 0:
        array = level_of(stream_key, shape, cuts, -0.22, 0.18) * array
    return jnp.clip(array, min=-bound, max=bound).astype(kind)


def setup_inputs(seed: int = 0) -> dict:
    seeds = jax.random.split(jax.random.key(seed), 8)
    return {
        "stream": noise(seeds[0], (TOKENS, D), 1.0, 6.0, ((1, 8),)),
        "gain_first": jnp.clip(1.0 + 0.1 * jax.random.normal(seeds[1], (D,), jnp.float32), 0.5, 1.5),
        "lift_first": noise(seeds[2], (D, HIDDEN_SIZE), D ** -0.5, 0.125, ((0, 8), (1, 4))),
        "drop_first": noise(seeds[3], (HIDDEN_SIZE, D), HIDDEN_SIZE ** -0.5, 0.0625, ((0, 4), (1, 8))),
        "gain_second": jnp.clip(1.0 + 0.1 * jax.random.normal(seeds[4], (D,), jnp.float32), 0.5, 1.5),
        "lift_second": noise(seeds[5], (D, HIDDEN_SIZE), D ** -0.5, 0.125, ((0, 8), (1, 4))),
        "drop_second": noise(seeds[6], (HIDDEN_SIZE, D), HIDDEN_SIZE ** -0.5, 0.0625, ((0, 4), (1, 8))),
    }


residual_scale = 0.25
epsilon = 1e-6


def sublayer(stream, gain_vector, lift_weight, drop_weight):
    feature_count = stream.shape[-1]
    widened = stream.astype(jnp.float32)
    squares = jnp.sum(widened * widened, axis=-1, keepdims=True)
    gained = (widened * gain_vector.astype(jnp.float32)).astype(jnp.bfloat16)
    pre_act = jnp.dot(gained, lift_weight, preferred_element_type=jnp.float32)
    pre_act = pre_act * lax.rsqrt(squares / feature_count + epsilon)
    hidden = jnp.square(jnp.maximum(pre_act, 0.0)).astype(jnp.bfloat16)
    branch = jnp.dot(hidden, drop_weight, preferred_element_type=jnp.float32)
    return (residual_scale * widened + branch).astype(jnp.bfloat16)


def reference(stream, gain_first, lift_first, drop_first, gain_second, lift_second, drop_second):
    middle = sublayer(stream, gain_first, lift_first, drop_first)
    return sublayer(middle, gain_second, lift_second, drop_second)
```

```python
import functools

import jax
import jax.numpy as jnp
from jax import lax
from jax.experimental import pallas as pl
from jax.experimental.pallas import tpu as pltpu
from jax.sharding import PartitionSpec as P

residual_scale = 0.25
epsilon = 1e-06
MESH = pl.DeviceIdType.MESH
EXT = 128
GROUPS = 2
TILE = 512


def split_of(count):
    best = 1
    for d in range(1, count + 1):
        if count % d == 0 and d * d <= count:
            best = d
    return best


def widened_block(value):
    return value.astype(jnp.float32)


def kernel(cfg, stream_ref, gain0, gain1, lift0_h, drop0_h, lift1_h, drop1_h, out_ref,
           lift0, drop0, lift1, drop1, s_buf, xsend, xrecv, pown, sqown, zsend, zrecv, hid,
           csend, crecv, ybuf,
           wsem, xs_sem, xr_sem, zs_sem, zr_sem, hzs, hzr, hxs, hxr, cs_sem, cr_sem, ys_sem, yr_sem):
    nz, nx, ny, nc, G, Tg, Tt, H, D = cfg
    r = lax.axis_index("ra")
    c = lax.axis_index("cb")
    z, x = r // nx, lax.rem(r, nx)
    y, core = c // nc, lax.rem(c, nc)

    loads = []
    for i, (src, dst) in enumerate(((lift0_h, lift0), (drop0_h, drop0), (lift1_h, lift1), (drop1_h, drop1))):
        cp = pltpu.make_async_copy(src, dst, wsem.at[i])
        cp.start()
        loads.append(cp)

    zp = [lax.rem(z + k, nz) for k in range(nz)]
    zm = [lax.rem(z + nz - k, nz) for k in range(nz)]
    xp = [lax.rem(x + m, nx) for m in range(nx)]
    xm = [lax.rem(x + nx - m, nx) for m in range(nx)]
    zdev = [(zp[k] * nx + x, c) for k in range(nz)]
    xdev = [(z * nx + xp[m], c) for m in range(nx)]
    cdev = (r, y * nc + lax.rem(core + 1, nc))
    ydev = [(r, lax.rem(y + j, ny) * nc + core) for j in range(ny)]
    peers = [zdev[k] for k in range(1, nz)] + [xdev[m] for m in range(1, nx)] + [cdev] + [ydev[j] for j in range(1, ny)]
    order = sorted(range(1, nz), key=lambda k: (abs(k - nz // 2), k))

    barrier = pltpu.get_barrier_semaphore()
    for dev in peers:
        pl.semaphore_signal(barrier, inc=1, device_id=dev, device_id_type=MESH)

    gains = (gain0, gain1)
    lifts = (lift0, lift1)
    drops = (drop0, drop1)
    half = nz * Tt
    pending = []

    def remote(src, dst, ssem, rsem, dev):
        cp = pltpu.make_async_remote_copy(src_ref=src, dst_ref=dst, send_sem=ssem, recv_sem=rsem,
                                          device_id=dev, device_id_type=MESH)
        cp.start()
        pending.append(cp)
        return cp

    lane = lax.broadcasted_iota(jnp.int32, (1, EXT), 1)

    def pack_sq(sq):
        hi = sq.astype(jnp.bfloat16).astype(jnp.float32)
        return jnp.where(lane < EXT // 2, hi, sq - hi).astype(jnp.bfloat16)

    def unpack_sq(ext):
        e = ext.astype(jnp.float32)
        return e[:, 0:1] + e[:, EXT // 2:EXT // 2 + 1]

    xcp, zcp, hzc, hxc, ccp, ycp = {}, {}, {}, {}, {}, {}

    def s1(l, g):
        gain = gains[l][...]
        w = lifts[l]
        for m in [*range(1, nx), 0]:
            rows = pl.ds(pl.multiple_of(xp[m] * half, half), half)
            s = s_buf[l, g, rows, :]
            sq = jnp.sum(s * s, axis=1, keepdims=True)
            gd = (s * gain).astype(jnp.bfloat16)
            if m == 0:
                for zz in range(nz):
                    sqown[l, g, zz] = jnp.broadcast_to(sq[zz * Tt:(zz + 1) * Tt], (Tt, EXT))
            else:
                ext = pack_sq(sq)
                for zz in range(nz):
                    xsend[l, g, m - 1, zz, :, H:] = ext[zz * Tt:(zz + 1) * Tt]
            for t in range(0, H, TILE):
                p = jnp.dot(gd, w[:, t:t + TILE], preferred_element_type=jnp.float32)
                for zz in range(nz):
                    part = p[zz * Tt:(zz + 1) * Tt]
                    if m == 0:
                        pown[l, g, zz, :, t:t + TILE] = part
                    else:
                        xsend[l, g, m - 1, zz, :, t:t + TILE] = part.astype(jnp.bfloat16)
            if m > 0:
                for k in order + [0]:
                    xcp[l, g, m, k] = remote(xsend.at[l, g, m - 1, zp[k]], xrecv.at[l, g, m - 1, zp[k]],
                                             xs_sem.at[l, g, m - 1, k], xr_sem.at[l, g, m - 1, k], xdev[m])

    def xsum(l, g, k):
        for m in range(1, nx):
            xcp[l, g, m, k].wait_recv()
        acc = pown[l, g, zp[k]]
        sq = sqown[l, g, zp[k]][:, 0:1]
        for m in range(1, nx):
            acc = acc + xrecv[l, g, m - 1, zp[k], :, :H].astype(jnp.float32)
            sq = sq + unpack_sq(xrecv[l, g, m - 1, zp[k], :, H:])
        return acc, sq

    def s2(l, g):
        for k in order:
            acc, sq = xsum(l, g, k)
            zsend[l, g, k - 1, :, :H] = acc.astype(jnp.bfloat16)
            zsend[l, g, k - 1, :, H:] = pack_sq(sq)
            zcp[l, g, k] = remote(zsend.at[l, g, k - 1], zrecv.at[l, g, k - 1],
                                  zs_sem.at[l, g, k - 1], zr_sem.at[l, g, k - 1], zdev[k])

    def s3(l, g):
        acc, sq = xsum(l, g, 0)
        for k in order:
            zcp[l, g, k].wait_recv()
            acc = acc + zrecv[l, g, k - 1, :, :H].astype(jnp.float32)
            sq = sq + unpack_sq(zrecv[l, g, k - 1, :, H:])
        pre = acc * lax.rsqrt(sq / D + epsilon)
        b = x * nz + z
        hid[l, g, b] = jnp.square(jnp.maximum(pre, 0.0)).astype(jnp.bfloat16)
        for k in order:
            hzc[l, g, k] = remote(hid.at[l, g, b], hid.at[l, g, b], hzs.at[l, g, k - 1], hzr.at[l, g, k - 1], zdev[k])
        for m in range(1, nx):
            hxc[l, g, m, 0] = remote(hid.at[l, g, b], hid.at[l, g, b], hxs.at[l, g, m - 1, 0], hxr.at[l, g, m - 1, 0], xdev[m])

    def s4(l, g):
        for k in order:
            hzc[l, g, k].wait_recv()
            b = x * nz + zm[k]
            for m in range(1, nx):
                hxc[l, g, m, k] = remote(hid.at[l, g, b], hid.at[l, g, b], hxs.at[l, g, m - 1, k], hxr.at[l, g, m - 1, k], xdev[m])

    def s5(l, g):
        for m in range(1, nx):
            for k in [0] + order:
                hxc[l, g, m, k].wait_recv()
        h = hid[l, g]
        if Tt % 16 == 0:
            h = h.reshape(Tg, H)
        else:
            h = h.astype(jnp.float32).reshape(Tg, H).astype(jnp.bfloat16)
        csend[l, g] = jnp.dot(h, drops[l][...], preferred_element_type=jnp.float32)
        ccp[l, g] = remote(csend.at[l, g], crecv.at[l, g], cs_sem.at[l, g], cr_sem.at[l, g], cdev)

    def s6(l, g):
        ccp[l, g].wait_recv()
        ybuf[l, g, y] = (csend[l, g] + crecv[l, g]).astype(jnp.bfloat16)
        for j in range(1, ny):
            ycp[l, g, j] = remote(ybuf.at[l, g, y], ybuf.at[l, g, y], ys_sem.at[l, g, j - 1], yr_sem.at[l, g, j - 1], ydev[j])

    def s7(l, g):
        for j in range(1, ny):
            ycp[l, g, j].wait_recv()
        total = ybuf[l, g, 0].astype(jnp.float32)
        for j in range(1, ny):
            total = total + ybuf[l, g, j].astype(jnp.float32)
        res = (residual_scale * s_buf[l, g] + total).astype(jnp.bfloat16)
        if l == 0:
            s_buf[1, g] = res.astype(jnp.float32)
        else:
            out_ref[g * Tg:(g + 1) * Tg, :] = res

    for g in range(G):
        s_buf[0, g] = stream_ref[g * Tg:(g + 1) * Tg, :].astype(jnp.float32)
    pl.semaphore_wait(barrier, len(peers))
    loads[0].wait()
    for g in range(G):
        s1(0, g)
    for l in range(2):
        for stage in (s2, s3, s4):
            for g in range(G):
                stage(l, g)
        if l == 0:
            for i in range(1, 4):
                loads[i].wait()
        for stage in (s5, s6):
            for g in range(G):
                stage(l, g)
        for g in range(G):
            s7(l, g)
            if l == 0:
                s1(1, g)
    for cp in pending:
        cp.wait_send()


def on_device(nra, ncb, stream, gain_first, lift_first, drop_first, gain_second, lift_second, drop_second):
    nx = split_of(nra)
    nz = nra // nx
    nc = 2
    ny = ncb // nc
    T, Dl = stream.shape
    H = lift_first.shape[1]
    G = GROUPS if T % (GROUPS * nra * 8) == 0 else 1
    Tg = T // G
    Tt = Tg // nra
    L = 2
    cfg = (nz, nx, ny, nc, G, Tg, Tt, H, Dl * nra)
    bf, f32 = jnp.bfloat16, jnp.float32
    dma = pltpu.SemaphoreType.DMA
    vm = pl.BlockSpec(memory_space=pltpu.VMEM)
    hbm = pl.BlockSpec(memory_space=pl.ANY)
    wide = H + EXT
    scratch = [
        pltpu.VMEM(lift_first.shape, bf), pltpu.VMEM(drop_first.shape, bf),
        pltpu.VMEM(lift_second.shape, bf), pltpu.VMEM(drop_second.shape, bf),
        pltpu.VMEM((L, G, Tg, Dl), f32),
        pltpu.VMEM((L, G, nx - 1, nz, Tt, wide), bf),
        pltpu.VMEM((L, G, nx - 1, nz, Tt, wide), bf),
        pltpu.VMEM((L, G, nz, Tt, H), f32),
        pltpu.VMEM((L, G, nz, Tt, EXT), f32),
        pltpu.VMEM((L, G, nz - 1, Tt, wide), bf),
        pltpu.VMEM((L, G, nz - 1, Tt, wide), bf),
        pltpu.VMEM((L, G, nra, Tt, H), bf),
        pltpu.VMEM((L, G, Tg, Dl), f32),
        pltpu.VMEM((L, G, Tg, Dl), f32),
        pltpu.VMEM((L, G, ny, Tg, Dl), bf),
        dma((4,)),
        dma((L, G, nx - 1, nz)), dma((L, G, nx - 1, nz)),
        dma((L, G, nz - 1)), dma((L, G, nz - 1)),
        dma((L, G, nz - 1)), dma((L, G, nz - 1)),
        dma((L, G, nx - 1, nz)), dma((L, G, nx - 1, nz)),
        dma((L, G)), dma((L, G)),
        dma((L, G, ny - 1)), dma((L, G, ny - 1)),
    ]
    return pl.pallas_call(
        functools.partial(kernel, cfg),
        out_shape=jax.ShapeDtypeStruct((T, Dl), bf),
        in_specs=[vm, vm, vm, hbm, hbm, hbm, hbm],
        out_specs=vm,
        scratch_shapes=scratch,
        compiler_params=pltpu.CompilerParams(collective_id=0, has_side_effects=True,
                                             vmem_limit_bytes=48 * 1024 * 1024),
    )(stream, gain_first.reshape(1, -1), gain_second.reshape(1, -1), lift_first, drop_first, lift_second, drop_second)


def solution(mesh):
    return jax.shard_map(
        functools.partial(on_device, mesh.shape["ra"], mesh.shape["cb"]),
        mesh=mesh,
        in_specs=(
            P(None, "ra"),
            P("ra"),
            P("ra", "cb"),
            P("cb", "ra"),
            P("ra"),
            P("ra", "cb"),
            P("cb", "ra"),
        ),
        out_specs=P(None, "ra"),
        check_vma=False,
    )
```

```python
import functools

import jax
import jax.numpy as jnp
from jax import lax
from jax.experimental import pallas as pl
from jax.experimental.pallas import tpu as pltpu
from jax.sharding import PartitionSpec as P

residual_scale = 0.25
epsilon = 1e-06
MESH = pl.DeviceIdType.MESH
EXT = 128
GROUPS = 2
TILE = 512
GRANT = 60 * 1024 * 1024


def split_of(count):
    best = 1
    for d in range(1, count + 1):
        if count % d == 0 and d * d <= count:
            best = d
    return best


def kernel(cfg, stream_h, gain0_h, gain1_h, lift0_h, drop0_h, lift1_h, drop1_h, out_ref,
           stream_ref, gain0, gain1, lift0, drop0, lift1, drop1, s_buf, xsend, xrecv, pown, sqown, zsend, zrecv, hid,
           csend, crecv, ybuf,
           wsem, xs_sem, xr_sem, zs_sem, zr_sem, hzs, hzr, hxs, hxr, cs_sem, cr_sem, ys_sem, yr_sem):
    nz, nx, ny, nc, G, Tg, Tt, H, D = cfg
    r = lax.axis_index("ra")
    c = lax.axis_index("cb")
    z, x = r // nx, lax.rem(r, nx)
    y, core = c // nc, lax.rem(c, nc)

    loads = []
    for i, (src, dst) in enumerate(((stream_h, stream_ref), (gain0_h, gain0), (lift0_h, lift0), (drop0_h, drop0),
                                (gain1_h, gain1), (lift1_h, lift1), (drop1_h, drop1))):
        cp = pltpu.make_async_copy(src, dst, wsem.at[i])
        cp.start()
        loads.append(cp)

    zp = [lax.rem(z + k, nz) for k in range(nz)]
    zm = [lax.rem(z + nz - k, nz) for k in range(nz)]
    xp = [lax.rem(x + m, nx) for m in range(nx)]
    xm = [lax.rem(x + nx - m, nx) for m in range(nx)]
    zdev = [(zp[k] * nx + x, c) for k in range(nz)]
    xdev = [(z * nx + xp[m], c) for m in range(nx)]
    cdev = (r, y * nc + lax.rem(core + 1, nc))
    ydev = [(r, lax.rem(y + j, ny) * nc + core) for j in range(ny)]
    peers = [zdev[k] for k in range(1, nz)] + [xdev[m] for m in range(1, nx)] + [cdev] + [ydev[j] for j in range(1, ny)]
    order = sorted(range(1, nz), key=lambda k: (abs(k - nz // 2), k))

    barrier = pltpu.get_barrier_semaphore()
    for dev in peers:
        pl.semaphore_signal(barrier, inc=1, device_id=dev, device_id_type=MESH)

    gains = (gain0, gain1)
    lifts = (lift0, lift1)
    drops = (drop0, drop1)
    half = nz * Tt
    pending = []

    def remote(src, dst, ssem, rsem, dev):
        cp = pltpu.make_async_remote_copy(src_ref=src, dst_ref=dst, send_sem=ssem, recv_sem=rsem,
                                          device_id=dev, device_id_type=MESH)
        cp.start()
        pending.append(cp)
        return cp

    lane = lax.broadcasted_iota(jnp.int32, (1, EXT), 1)

    def pack_sq(sq):
        hi = sq.astype(jnp.bfloat16).astype(jnp.float32)
        return jnp.where(lane < EXT // 2, hi, sq - hi).astype(jnp.bfloat16)

    def unpack_sq(ext):
        e = ext.astype(jnp.float32)
        return e[:, 0:1] + e[:, EXT // 2:EXT // 2 + 1]

    xcp, zcp, hzc, hxc, ccp, ycp = {}, {}, {}, {}, {}, {}

    def s1(l, g):
        gain = gains[l][...]
        w = lifts[l]
        for m in [*range(1, nx), 0]:
            rows = pl.ds(pl.multiple_of(xp[m] * half, half), half)
            s = s_buf[l, g, rows, :]
            sq = jnp.sum(s * s, axis=1, keepdims=True)
            gd = (s * gain).astype(jnp.bfloat16)
            if m == 0:
                for zz in range(nz):
                    sqown[l, g, zz] = jnp.broadcast_to(sq[zz * Tt:(zz + 1) * Tt], (Tt, EXT))
            else:
                ext = pack_sq(sq)
                for zz in range(nz):
                    xsend[l, g, m - 1, zz, :, H:] = ext[zz * Tt:(zz + 1) * Tt]
            for t in range(0, H, TILE):
                p = jnp.dot(gd, w[:, t:t + TILE], preferred_element_type=jnp.float32)
                for zz in range(nz):
                    part = p[zz * Tt:(zz + 1) * Tt]
                    if m == 0:
                        pown[l, g, zz, :, t:t + TILE] = part
                    else:
                        xsend[l, g, m - 1, zz, :, t:t + TILE] = part.astype(jnp.bfloat16)
            if m > 0:
                for k in order + [0]:
                    xcp[l, g, m, k] = remote(xsend.at[l, g, m - 1, zp[k]], xrecv.at[l, g, m - 1, zp[k]],
                                             xs_sem.at[l, g, m - 1, k], xr_sem.at[l, g, m - 1, k], xdev[m])

    def xsum(l, g, k):
        for m in range(1, nx):
            xcp[l, g, m, k].wait_recv()
        acc = pown[l, g, zp[k]]
        sq = sqown[l, g, zp[k]][:, 0:1]
        for m in range(1, nx):
            acc = acc + xrecv[l, g, m - 1, zp[k], :, :H].astype(jnp.float32)
            sq = sq + unpack_sq(xrecv[l, g, m - 1, zp[k], :, H:])
        return acc, sq

    def s2(l, g):
        for k in order:
            acc, sq = xsum(l, g, k)
            zsend[l, g, k - 1, :, :H] = acc.astype(jnp.bfloat16)
            zsend[l, g, k - 1, :, H:] = pack_sq(sq)
            zcp[l, g, k] = remote(zsend.at[l, g, k - 1], zrecv.at[l, g, k - 1],
                                  zs_sem.at[l, g, k - 1], zr_sem.at[l, g, k - 1], zdev[k])

    def s3(l, g):
        acc, sq = xsum(l, g, 0)
        for k in order:
            zcp[l, g, k].wait_recv()
            acc = acc + zrecv[l, g, k - 1, :, :H].astype(jnp.float32)
            sq = sq + unpack_sq(zrecv[l, g, k - 1, :, H:])
        pre = acc * lax.rsqrt(sq / D + epsilon)
        b = x * nz + z
        hid[l, g, b] = jnp.square(jnp.maximum(pre, 0.0)).astype(jnp.bfloat16)
        for k in order:
            hzc[l, g, k] = remote(hid.at[l, g, b], hid.at[l, g, b], hzs.at[l, g, k - 1], hzr.at[l, g, k - 1], zdev[k])
        for m in range(1, nx):
            hxc[l, g, m, 0] = remote(hid.at[l, g, b], hid.at[l, g, b], hxs.at[l, g, m - 1, 0], hxr.at[l, g, m - 1, 0], xdev[m])

    def s4(l, g):
        for k in order:
            hzc[l, g, k].wait_recv()
            b = x * nz + zm[k]
            for m in range(1, nx):
                hxc[l, g, m, k] = remote(hid.at[l, g, b], hid.at[l, g, b], hxs.at[l, g, m - 1, k], hxr.at[l, g, m - 1, k], xdev[m])

    def s5(l, g):
        for m in range(1, nx):
            for k in [0] + order:
                hxc[l, g, m, k].wait_recv()
        h = hid[l, g]
        if Tt % 16 == 0:
            h = h.reshape(Tg, H)
        else:
            h = h.astype(jnp.float32).reshape(Tg, H).astype(jnp.bfloat16)
        csend[l, g] = jnp.dot(h, drops[l][...], preferred_element_type=jnp.float32)
        ccp[l, g] = remote(csend.at[l, g], crecv.at[l, g], cs_sem.at[l, g], cr_sem.at[l, g], cdev)

    def s6(l, g):
        ccp[l, g].wait_recv()
        ybuf[l, g, y] = (csend[l, g] + crecv[l, g]).astype(jnp.bfloat16)
        for j in range(1, ny):
            ycp[l, g, j] = remote(ybuf.at[l, g, y], ybuf.at[l, g, y], ys_sem.at[l, g, j - 1], yr_sem.at[l, g, j - 1], ydev[j])

    def s7(l, g):
        for j in range(1, ny):
            ycp[l, g, j].wait_recv()
        total = ybuf[l, g, 0].astype(jnp.float32)
        for j in range(1, ny):
            total = total + ybuf[l, g, j].astype(jnp.float32)
        res = (residual_scale * s_buf[l, g] + total).astype(jnp.bfloat16)
        if l == 0:
            s_buf[1, g] = res.astype(jnp.float32)
        else:
            out_ref[g * Tg:(g + 1) * Tg, :] = res

    loads[0].wait()
    for g in range(G):
        s_buf[0, g] = stream_ref[g * Tg:(g + 1) * Tg, :].astype(jnp.float32)
    loads[1].wait()
    loads[2].wait()
    pl.semaphore_wait(barrier, len(peers))
    for g in range(G):
        s1(0, g)
    for l in range(2):
        for stage in (s2, s3, s4):
            for g in range(G):
                stage(l, g)
        if l == 0:
            for i in range(3, 7):
                loads[i].wait()
        for stage in (s5, s6):
            for g in range(G):
                stage(l, g)
        for g in range(G):
            s7(l, g)
            if l == 0:
                s1(1, g)
    for cp in pending:
        cp.wait_send()


def on_device(nra, ncb, stream, gain_first, lift_first, drop_first, gain_second, lift_second, drop_second):
    nx = split_of(nra)
    nz = nra // nx
    nc = 2
    ny = ncb // nc
    T, Dl = stream.shape
    H = lift_first.shape[1]
    G = GROUPS if T % (GROUPS * nra * 8) == 0 else 1
    Tg = T // G
    Tt = Tg // nra
    L = 2
    cfg = (nz, nx, ny, nc, G, Tg, Tt, H, Dl * nra)
    bf, f32 = jnp.bfloat16, jnp.float32
    dma = pltpu.SemaphoreType.DMA
    vm = pl.BlockSpec(memory_space=pltpu.VMEM)
    hbm = pl.BlockSpec(memory_space=pl.ANY)
    wide = H + EXT
    scratch = [
        pltpu.VMEM((T, Dl), bf), pltpu.VMEM((1, Dl), f32), pltpu.VMEM((1, Dl), f32),
        pltpu.VMEM(lift_first.shape, bf), pltpu.VMEM(drop_first.shape, bf),
        pltpu.VMEM(lift_second.shape, bf), pltpu.VMEM(drop_second.shape, bf),
        pltpu.VMEM((L, G, Tg, Dl), f32),
        pltpu.VMEM((L, G, nx - 1, nz, Tt, wide), bf),
        pltpu.VMEM((L, G, nx - 1, nz, Tt, wide), bf),
        pltpu.VMEM((L, G, nz, Tt, H), f32),
        pltpu.VMEM((L, G, nz, Tt, EXT), f32),
        pltpu.VMEM((L, G, nz - 1, Tt, wide), bf),
        pltpu.VMEM((L, G, nz - 1, Tt, wide), bf),
        pltpu.VMEM((L, G, nra, Tt, H), bf),
        pltpu.VMEM((L, G, Tg, Dl), f32),
        pltpu.VMEM((L, G, Tg, Dl), f32),
        pltpu.VMEM((L, G, ny, Tg, Dl), bf),
        dma((7,)),
        dma((L, G, nx - 1, nz)), dma((L, G, nx - 1, nz)),
        dma((L, G, nz - 1)), dma((L, G, nz - 1)),
        dma((L, G, nz - 1)), dma((L, G, nz - 1)),
        dma((L, G, nx - 1, nz)), dma((L, G, nx - 1, nz)),
        dma((L, G)), dma((L, G)),
        dma((L, G, ny - 1)), dma((L, G, ny - 1)),
    ]
    return pl.pallas_call(
        functools.partial(kernel, cfg),
        out_shape=jax.ShapeDtypeStruct((T, Dl), bf),
        in_specs=[hbm] * 7,
        out_specs=vm,
        scratch_shapes=scratch,
        compiler_params=pltpu.CompilerParams(collective_id=0, has_side_effects=True,
                                             vmem_limit_bytes=GRANT),
    )(stream, gain_first.reshape(1, -1), gain_second.reshape(1, -1), lift_first, drop_first, lift_second, drop_second)


def solution(mesh):
    return jax.shard_map(
        functools.partial(on_device, mesh.shape["ra"], mesh.shape["cb"]),
        mesh=mesh,
        in_specs=(
            P(None, "ra"),
            P("ra"),
            P("ra", "cb"),
            P("cb", "ra"),
            P("ra"),
            P("ra", "cb"),
            P("cb", "ra"),
        ),
        out_specs=P(None, "ra"),
        check_vma=False,
    )
```

```python
import functools

import jax
import jax.numpy as jnp
from jax import lax
from jax.experimental import pallas as pl
from jax.experimental.pallas import tpu as pltpu
from jax.sharding import PartitionSpec as P

residual_scale = 0.25
epsilon = 1e-06
MESH = pl.DeviceIdType.MESH
EXT = 128
GROUPS = 2
TILE = 512
GRANT = 60 * 1024 * 1024


def split_of(count):
    best = 1
    for d in range(1, count + 1):
        if count % d == 0 and d * d <= count:
            best = d
    return best


def kernel(cfg, stream_h, gain0_h, gain1_h, lift0_h, drop0_h, lift1_h, drop1_h, out_ref,
           stream_ref, gain0, gain1, lift0, drop0, lift1, drop1, s_buf, xsend, xrecv, pown, sqown, zsend, zrecv, hid,
           ybuf,
           wsem, xs_sem, xr_sem, zs_sem, zr_sem, hzs, hzr, hxs, hxr, ys_sem, yr_sem):
    nz, nx, ny, G, Tg, Tt, H, D = cfg
    r = lax.axis_index("ra")
    c = lax.axis_index("cb")
    z, x = r // nx, lax.rem(r, nx)

    loads = []
    for i, (src, dst) in enumerate(((stream_h, stream_ref), (gain0_h, gain0), (lift0_h, lift0), (drop0_h, drop0),
                                (gain1_h, gain1), (lift1_h, lift1), (drop1_h, drop1))):
        cp = pltpu.make_async_copy(src, dst, wsem.at[i])
        cp.start()
        loads.append(cp)

    zp = [lax.rem(z + k, nz) for k in range(nz)]
    zm = [lax.rem(z + nz - k, nz) for k in range(nz)]
    xp = [lax.rem(x + m, nx) for m in range(nx)]
    xm = [lax.rem(x + nx - m, nx) for m in range(nx)]
    zdev = [(zp[k] * nx + x, c) for k in range(nz)]
    xdev = [(z * nx + xp[m], c) for m in range(nx)]
    ydev = [(r, lax.rem(c + j, ny)) for j in range(ny)]
    peers = [zdev[k] for k in range(1, nz)] + [xdev[m] for m in range(1, nx)] + [ydev[j] for j in range(1, ny)]
    order = sorted(range(1, nz), key=lambda k: (abs(k - nz // 2), k))

    barrier = pltpu.get_barrier_semaphore()
    for dev in peers:
        pl.semaphore_signal(barrier, inc=1, device_id=dev, device_id_type=MESH)

    gains = (gain0, gain1)
    lifts = (lift0, lift1)
    drops = (drop0, drop1)
    half = nz * Tt
    pending = []

    def remote(src, dst, ssem, rsem, dev):
        cp = pltpu.make_async_remote_copy(src_ref=src, dst_ref=dst, send_sem=ssem, recv_sem=rsem,
                                          device_id=dev, device_id_type=MESH)
        cp.start()
        pending.append(cp)
        return cp

    lane = lax.broadcasted_iota(jnp.int32, (1, EXT), 1)

    def pack_sq(sq):
        hi = sq.astype(jnp.bfloat16).astype(jnp.float32)
        return jnp.where(lane < EXT // 2, hi, sq - hi).astype(jnp.bfloat16)

    def unpack_sq(ext):
        e = ext.astype(jnp.float32)
        return e[:, 0:1] + e[:, EXT // 2:EXT // 2 + 1]

    xcp, zcp, hzc, hxc, ycp = {}, {}, {}, {}, {}

    def s1(l, g):
        gain = gains[l][...]
        w = lifts[l]
        for m in [*range(1, nx), 0]:
            rows = pl.ds(pl.multiple_of(xp[m] * half, half), half)
            s = s_buf[l, g, rows, :]
            sq = jnp.sum(s * s, axis=1, keepdims=True)
            gd = (s * gain).astype(jnp.bfloat16)
            if m == 0:
                for zz in range(nz):
                    sqown[l, g, zz] = jnp.broadcast_to(sq[zz * Tt:(zz + 1) * Tt], (Tt, EXT))
            else:
                ext = pack_sq(sq)
                for zz in range(nz):
                    xsend[l, g, m - 1, zz, :, H:] = ext[zz * Tt:(zz + 1) * Tt]
            for t in range(0, H, TILE):
                p = jnp.dot(gd, w[:, t:t + TILE], preferred_element_type=jnp.float32)
                for zz in range(nz):
                    part = p[zz * Tt:(zz + 1) * Tt]
                    if m == 0:
                        pown[l, g, zz, :, t:t + TILE] = part
                    else:
                        xsend[l, g, m - 1, zz, :, t:t + TILE] = part.astype(jnp.bfloat16)
            if m > 0:
                if l == 0 and g == 0 and m == 1:
                    pl.semaphore_wait(barrier, len(peers))
                for k in order + [0]:
                    xcp[l, g, m, k] = remote(xsend.at[l, g, m - 1, zp[k]], xrecv.at[l, g, m - 1, zp[k]],
                                             xs_sem.at[l, g, m - 1, k], xr_sem.at[l, g, m - 1, k], xdev[m])

    def xsum(l, g, k):
        for m in range(1, nx):
            xcp[l, g, m, k].wait_recv()
        acc = pown[l, g, zp[k]]
        sq = sqown[l, g, zp[k]][:, 0:1]
        for m in range(1, nx):
            acc = acc + xrecv[l, g, m - 1, zp[k], :, :H].astype(jnp.float32)
            sq = sq + unpack_sq(xrecv[l, g, m - 1, zp[k], :, H:])
        return acc, sq

    def s2(l, g):
        for k in order:
            acc, sq = xsum(l, g, k)
            zsend[l, g, k - 1, :, :H] = acc.astype(jnp.bfloat16)
            zsend[l, g, k - 1, :, H:] = pack_sq(sq)
            zcp[l, g, k] = remote(zsend.at[l, g, k - 1], zrecv.at[l, g, k - 1],
                                  zs_sem.at[l, g, k - 1], zr_sem.at[l, g, k - 1], zdev[k])

    def s3(l, g):
        acc, sq = xsum(l, g, 0)
        for k in order:
            zcp[l, g, k].wait_recv()
            acc = acc + zrecv[l, g, k - 1, :, :H].astype(jnp.float32)
            sq = sq + unpack_sq(zrecv[l, g, k - 1, :, H:])
        pre = acc * lax.rsqrt(sq / D + epsilon)
        b = x * nz + z
        hid[l, g, b] = jnp.square(jnp.maximum(pre, 0.0)).astype(jnp.bfloat16)
        for k in order:
            hzc[l, g, k] = remote(hid.at[l, g, b], hid.at[l, g, b], hzs.at[l, g, k - 1], hzr.at[l, g, k - 1], zdev[k])
        for m in range(1, nx):
            hxc[l, g, m, 0] = remote(hid.at[l, g, b], hid.at[l, g, b], hxs.at[l, g, m - 1, 0], hxr.at[l, g, m - 1, 0], xdev[m])

    def s4(l, g):
        for k in order:
            hzc[l, g, k].wait_recv()
            b = x * nz + zm[k]
            for m in range(1, nx):
                hxc[l, g, m, k] = remote(hid.at[l, g, b], hid.at[l, g, b], hxs.at[l, g, m - 1, k], hxr.at[l, g, m - 1, k], xdev[m])

    def s5(l, g):
        for m in range(1, nx):
            for k in [0] + order:
                hxc[l, g, m, k].wait_recv()
        h = hid[l, g]
        if Tt % 16 == 0:
            h = h.reshape(Tg, H)
        else:
            h = h.astype(jnp.float32).reshape(Tg, H).astype(jnp.bfloat16)
        ybuf[l, g, c] = jnp.dot(h, drops[l][...], preferred_element_type=jnp.float32).astype(jnp.bfloat16)
        for j in range(1, ny):
            ycp[l, g, j] = remote(ybuf.at[l, g, c], ybuf.at[l, g, c], ys_sem.at[l, g, j - 1], yr_sem.at[l, g, j - 1], ydev[j])

    def s7(l, g):
        for j in range(1, ny):
            ycp[l, g, j].wait_recv()
        total = ybuf[l, g, 0].astype(jnp.float32)
        for j in range(1, ny):
            total = total + ybuf[l, g, j].astype(jnp.float32)
        res = (residual_scale * s_buf[l, g] + total).astype(jnp.bfloat16)
        if l == 0:
            s_buf[1, g] = res.astype(jnp.float32)
        else:
            out_ref[g * Tg:(g + 1) * Tg, :] = res

    loads[0].wait()
    for g in range(G):
        s_buf[0, g] = stream_ref[g * Tg:(g + 1) * Tg, :].astype(jnp.float32)
    loads[1].wait()
    loads[2].wait()
    for g in range(G):
        s1(0, g)
    for l in range(2):
        for stage in (s2, s3, s4):
            for g in range(G):
                stage(l, g)
        if l == 0:
            for i in range(3, 7):
                loads[i].wait()
        for stage in (s5,):
            for g in range(G):
                stage(l, g)
        for g in range(G):
            s7(l, g)
            if l == 0:
                s1(1, g)
    for cp in pending:
        cp.wait_send()


def on_device(nra, ncb, stream, gain_first, lift_first, drop_first, gain_second, lift_second, drop_second):
    nx = split_of(nra)
    nz = nra // nx
    ny = ncb
    T, Dl = stream.shape
    H = lift_first.shape[1]
    G = GROUPS if T % (GROUPS * nra * 8) == 0 else 1
    Tg = T // G
    Tt = Tg // nra
    L = 2
    cfg = (nz, nx, ny, G, Tg, Tt, H, Dl * nra)
    bf, f32 = jnp.bfloat16, jnp.float32
    dma = pltpu.SemaphoreType.DMA
    vm = pl.BlockSpec(memory_space=pltpu.VMEM)
    hbm = pl.BlockSpec(memory_space=pl.ANY)
    wide = H + EXT
    scratch = [
        pltpu.VMEM((T, Dl), bf), pltpu.VMEM((1, Dl), f32), pltpu.VMEM((1, Dl), f32),
        pltpu.VMEM(lift_first.shape, bf), pltpu.VMEM(drop_first.shape, bf),
        pltpu.VMEM(lift_second.shape, bf), pltpu.VMEM(drop_second.shape, bf),
        pltpu.VMEM((L, G, Tg, Dl), f32),
        pltpu.VMEM((L, G, nx - 1, nz, Tt, wide), bf),
        pltpu.VMEM((L, G, nx - 1, nz, Tt, wide), bf),
        pltpu.VMEM((L, G, nz, Tt, H), f32),
        pltpu.VMEM((L, G, nz, Tt, EXT), f32),
        pltpu.VMEM((L, G, nz - 1, Tt, wide), bf),
        pltpu.VMEM((L, G, nz - 1, Tt, wide), bf),
        pltpu.VMEM((L, G, nra, Tt, H), bf),
        pltpu.VMEM((L, G, ny, Tg, Dl), bf),
        dma((7,)),
        dma((L, G, nx - 1, nz)), dma((L, G, nx - 1, nz)),
        dma((L, G, nz - 1)), dma((L, G, nz - 1)),
        dma((L, G, nz - 1)), dma((L, G, nz - 1)),
        dma((L, G, nx - 1, nz)), dma((L, G, nx - 1, nz)),
        dma((L, G, ny - 1)), dma((L, G, ny - 1)),
    ]
    return pl.pallas_call(
        functools.partial(kernel, cfg),
        out_shape=jax.ShapeDtypeStruct((T, Dl), bf),
        in_specs=[hbm] * 7,
        out_specs=vm,
        scratch_shapes=scratch,
        compiler_params=pltpu.CompilerParams(collective_id=0, has_side_effects=True,
                                             vmem_limit_bytes=GRANT),
    )(stream, gain_first.reshape(1, -1), gain_second.reshape(1, -1), lift_first, drop_first, lift_second, drop_second)


def solution(mesh):
    return jax.shard_map(
        functools.partial(on_device, mesh.shape["ra"], mesh.shape["cb"]),
        mesh=mesh,
        in_specs=(
            P(None, "ra"),
            P("ra"),
            P("ra", "cb"),
            P("cb", "ra"),
            P("ra"),
            P("ra", "cb"),
            P("cb", "ra"),
        ),
        out_specs=P(None, "ra"),
        check_vma=False,
    )
```
